32 devices in a mesh: grp: 2 (over y), fs: 4 (over z), tp: 4 (over x, core).
Axes of the slice: x: 2, y: 2, z: 4, core: 2. Of those that a mesh axis runs over, the one named last changes fastest.
Arguments:
- tokens: bfloat16 [8192, 2048], P(('grp', 'fs', 'tp')), parts along dimension 0, may hold values from -6 to 6
- first_gain: float32 [2048], replicated, may hold values from 0.1 to 1.9
- mixer_gain: float32 [2048], replicated, may hold values from 0.1 to 1.9
- gate_weight: bfloat16 [2048, 4608], P('fs', 'tp'), may hold values from -0.125 to 0.125
- up_weight: bfloat16 [2048, 4608], P('fs', 'tp'), may hold values from -0.125 to 0.125
- down_weight: bfloat16 [4608, 2048], P('tp', 'fs'), may hold values from -0.09375 to 0.09375
- query_weight: bfloat16 [2048, 2048], P('fs', 'tp'), may hold values from -0.125 to 0.125
- key_weight: bfloat16 [2048, 2048], P('fs', 'tp'), may hold values from -0.125 to 0.125
- value_weight: bfloat16 [2048, 4096], P('fs', 'tp'), may hold values from -0.125 to 0.125
- head_gain: float32 [4096], P('tp'), may hold values from 0.1 to 1.9
- out_weight: bfloat16 [4096, 2048], P('tp', 'fs'), may hold values from -0.09375 to 0.09375
- log_decay: float32 [2, 8], P(None, 'tp'), may hold values from -0.03125 to 0, as said below
Outputs:
- updated: bfloat16 [8192, 2048], P(('grp', 'fs', 'tp')), parts along dimension 0
The draws below stay inside these ranges and needn't reach their ends.
There are 2 independent parts, one for each index of `grp`. The reference program is written for one: setup_inputs(seed, part) draws one part's arguments, and reference() takes and returns one part's arrays. A program takes and returns all parts, laid end to end along the dimension named above; an argument that names none is the same for every part. Nothing has to cross between parts.
Inputs may be any that keep to these rules, and one draw needn't show every extreme that they name: `log_decay`: log decay per step of each direction (forward, then backward) and head.
All inputs are finite; a program needn't handle non-finite values.
Results may differ from the reference program's by a relative error of at most 0.02.
Values may be sent and summed in bfloat16 or wider, within the bound.
No kernel may reach another device: no remote copies, remote signals or barrier semaphores. Data moves between devices by JAX's collectives and lax.ppermute only.
A program may use at most 64 MiB of HBM per device.

```python
import math
import jax
import jax.numpy as jnp
from jax import lax

D = 2048
H = 8
DK = 256
DV = 512
FF = 4608
BLOCK = 128
TOK = 1024
TOKENS = 4096
N_TP = 4


def draw_log_decay(key, part):
    order = jax.random.permutation(jax.random.fold_in(key, 11), H)
    fast_count = H // 2
    fast_heads = order < fast_count
    unit = jax.random.uniform(jax.random.fold_in(key, 12), (2, H), jnp.float32)
    slow_rate = math.log(0.1) / TOK * (0.1 + 0.9 * unit)
    fast_rate = -4.0 / BLOCK + unit * (4.0 / BLOCK - 4.0 / (3.0 * BLOCK))
    return jnp.where(fast_heads[None, :], fast_rate, slow_rate).astype(jnp.float32)


def block_scale(stream_key, shape, cuts, smallest, top_value):
    level, own = 1.0, jax.random.fold_in(stream_key, 6)
    for position, parts in cuts:
        heights = jnp.exp(jax.random.uniform(jax.random.fold_in(own, position), (parts,), jnp.float32, smallest / len(cuts), top_value / len(cuts)))
        level = level * jnp.repeat(heights, shape[position] // parts).reshape([-1 if axis == position else 1 for axis in range(len(shape))])
    return level


def centred(own_key, dims, scale, limit, cuts=(), held_as=jnp.bfloat16):
    level = block_scale(own_key, dims, cuts, -0.22, 0.18) if cuts else 1.0
    drawn = jax.random.normal(own_key, dims, jnp.float32) * scale * level
    return jnp.minimum(jnp.maximum(drawn, -limit), limit).astype(held_as)


def setup_inputs(seed: int = 0, part: int = 0) -> dict:
    arg_keys = jax.random.split(jax.random.key(seed), 13)
    part_splits = jax.random.split(jax.random.fold_in(arg_keys[12], part), 13)
    tokens = centred(part_splits[0], (TOKENS, D), 1.0, 6.0, ((0, 16),))
    first_gain = jnp.clip(1.0 + 0.18 * jax.random.normal(arg_keys[1], (D,), jnp.float32), 0.1, 1.9)
    mixer_gain = jnp.clip(1.0 + 0.18 * jax.random.normal(arg_keys[2], (D,), jnp.float32), 0.1, 1.9)
    gate_weight = centred(arg_keys[3], (D, FF), D ** -0.5, 0.125, ((0, 4), (1, 4)))
    up_weight = centred(arg_keys[4], (D, FF), D ** -0.5, 0.125, ((0, 4), (1, 4)))
    down_weight = centred(arg_keys[5], (FF, D), FF ** -0.5, 0.09375, ((0, 4), (1, 4)))
    query_weight = centred(arg_keys[6], (D, H * DK), D ** -0.5, 0.125, ((0, 4), (1, 4)))
    key_weight = centred(arg_keys[7], (D, H * DK), D ** -0.5, 0.125, ((0, 4), (1, 4)))
    value_weight = centred(arg_keys[8], (D, H * DV), D ** -0.5, 0.125, ((0, 4), (1, 4)))
    head_gain = jnp.clip(1.0 + 0.18 * jax.random.normal(arg_keys[9], (H * DV,), jnp.float32), 0.1, 1.9)
    out_weight = centred(arg_keys[10], (H * DV, D), (H * DV) ** -0.5, 0.09375, ((0, 4), (1, 4)))
    log_decay = draw_log_decay(jax.random.fold_in(arg_keys[12], 71), part)
    return {"tokens": tokens, "first_gain": first_gain, "mixer_gain": mixer_gain, "gate_weight": gate_weight, "up_weight": up_weight, "down_weight": down_weight, "query_weight": query_weight, "key_weight": key_weight, "value_weight": value_weight, "head_gain": head_gain, "out_weight": out_weight, "log_decay": log_decay}


EPS = 1e-06

def norm_rows(values, gain):
    widened = values.astype(jnp.float32)
    factor = lax.rsqrt(lax.optimization_barrier(jnp.mean(widened * widened, axis=-1, keepdims=True)) + EPS)
    return (widened * factor * gain).astype(jnp.bfloat16)

def split_sum(left, right, pieces):
    width = left.shape[1] // pieces
    running = jnp.zeros((left.shape[0], right.shape[1]), jnp.float32)
    for which_block in range(pieces):
        product = jnp.dot(left[:, which_block * width:(which_block + 1) * width], right[which_block * width:(which_block + 1) * width], preferred_element_type=jnp.float32)
        running = running + lax.optimization_barrier(product.astype(jnp.bfloat16)).astype(jnp.float32)
    return running

def sweep_one(queries, key_rows, value_rows, log_rate):
    length = queries.shape[0]
    block_count = length // BLOCK
    places = jnp.arange(BLOCK, dtype=jnp.float32)
    distance = places[:, None] - places[None, :]
    inner_decay = jnp.where(distance >= 0, jnp.exp(log_rate * jnp.maximum(distance, 0.0)), 0.0)
    enter_decay = jnp.exp(log_rate * (places + 1.0))
    leave_decay = jnp.exp(log_rate * (BLOCK - 1.0 - places))
    block_decay = jnp.exp(log_rate * BLOCK)
    highest = lax.Precision.HIGHEST

    def advance(memory, blocks):
        query_block, key_block, value_block = blocks
        scores = jnp.dot(query_block.astype(jnp.bfloat16), key_block.astype(jnp.bfloat16).T, preferred_element_type=jnp.float32) * inner_decay
        result = jnp.dot(scores, value_block, precision=highest)
        result = result + jnp.dot(query_block, memory, precision=highest) * enter_decay[:, None]
        memory = memory * block_decay + jnp.dot((key_block * leave_decay[:, None]).T, value_block, precision=highest)
        return (memory, result)
    start_memory = jnp.zeros((queries.shape[1], value_rows.shape[1]), jnp.float32)
    _, results = lax.scan(advance, start_memory, (queries.reshape(block_count, BLOCK, -1), key_rows.reshape(block_count, BLOCK, -1), value_rows.reshape(block_count, BLOCK, -1)))
    return results.reshape(length, -1)

def retain_both(queries, key_rows, value_rows, forward_rate, backward_rate):
    forward_part = sweep_one(queries, key_rows, value_rows, forward_rate)
    backward_part = sweep_one(jnp.flip(queries, axis=0), jnp.flip(key_rows, axis=0), jnp.flip(value_rows, axis=0), backward_rate)
    return forward_part + jnp.flip(backward_part, axis=0)

def head_norm(outputs, gain):
    heads_here = gain.shape[0] // DV
    centered = outputs - lax.optimization_barrier(jnp.mean(outputs, axis=-1, keepdims=True))
    variance = lax.optimization_barrier(jnp.mean(centered * centered, axis=-1, keepdims=True))
    return centered * lax.rsqrt(variance + EPS) * gain.reshape(heads_here, 1, DV)

def feed_half(residual, gain, gate_weight, up_weight, down_weight):
    normed = norm_rows(residual, gain)
    gate_sum = jnp.dot(normed, gate_weight, preferred_element_type=jnp.float32)
    up_sum = jnp.dot(normed, up_weight, preferred_element_type=jnp.float32)
    hidden = (jax.nn.silu(gate_sum) * up_sum).astype(jnp.bfloat16)
    branch = split_sum(hidden, down_weight, N_TP)
    return (residual.astype(jnp.float32) + 0.5 * branch).astype(jnp.bfloat16)

def to_heads(values, width):
    widened = lax.optimization_barrier(values.astype(jnp.bfloat16)).astype(jnp.float32)
    return widened.reshape(-1, TOK, H, width).transpose(0, 2, 1, 3)

def mix_tokens(residual, gain, query_weight, key_weight, value_weight, head_gain, out_weight, log_decay):
    normed = norm_rows(residual, gain)
    queries = to_heads(jnp.dot(normed, query_weight, preferred_element_type=jnp.float32), DK) * DK ** (-0.5)
    key_rows = to_heads(jnp.dot(normed, key_weight, preferred_element_type=jnp.float32), DK)
    value_rows = to_heads(jnp.dot(normed, value_weight, preferred_element_type=jnp.float32), DV)

    def per_sequence(blocks):
        return jax.vmap(retain_both)(blocks[0], blocks[1], blocks[2], log_decay[0], log_decay[1])
    outputs = lax.map(per_sequence, (queries, key_rows, value_rows))
    normed_heads = head_norm(outputs, head_gain).astype(jnp.bfloat16)
    flat = normed_heads.transpose(0, 2, 1, 3).reshape(-1, H * DV)
    branch = split_sum(flat, out_weight, N_TP)
    return (residual.astype(jnp.float32) + branch).astype(jnp.bfloat16)

def reference(tokens, first_gain, mixer_gain, gate_weight, up_weight, down_weight, query_weight, key_weight, value_weight, head_gain, out_weight, log_decay):
    after_first = feed_half(tokens, first_gain, gate_weight, up_weight, down_weight)
    return mix_tokens(after_first, mixer_gain, query_weight, key_weight, value_weight, head_gain, out_weight, log_decay)
```

```python
import functools

import jax
import jax.numpy as jnp
from jax import lax
from jax.experimental import pallas as pl
from jax.experimental.pallas import tpu as pltpu
from jax.sharding import PartitionSpec as P

DK = 256
DV = 512
EPS = 1e-06


def norm_rows(values, gain):
    widened = values.astype(jnp.float32)
    factor = lax.rsqrt(jnp.mean(widened * widened, axis=-1, keepdims=True) + EPS)
    return (widened * factor * gain).astype(jnp.bfloat16)


def matmul(left, right):
    return jnp.dot(left, right, preferred_element_type=jnp.float32)


def chip_shift(value, chips, shift):
    pairs = [
        (((chip + shift) % chips) * 2 + core, chip * 2 + core)
        for chip in range(chips)
        for core in range(2)
    ]
    return lax.ppermute(value, "tp", pairs)


def core_swap(value, chips):
    return lax.ppermute(value, "tp", [(at, at ^ 1) for at in range(2 * chips)])


def chunk_ids(chips):
    at = lax.axis_index("tp")
    chip, core = at // 2, at % 2
    ahead = (chip + jnp.arange(chips, dtype=jnp.int32)) % chips
    return jnp.concatenate([ahead * 2 + core, ahead * 2 + 1 - core]).astype(jnp.int32)


def gather_rows(own, chips):
    same = [own] + [chip_shift(own, chips, shift) for shift in range(1, chips)]
    other = [core_swap(piece, chips) for piece in same]
    return jnp.concatenate(same + other, axis=0)


def scatter_sum(same_core, other_core, chips):
    swapped = core_swap(other_core, chips)
    summed = same_core.astype(jnp.float32) + swapped.astype(jnp.float32)
    rows = summed.shape[0] // chips
    total = summed[:rows]
    for shift in range(1, chips):
        piece = summed[shift * rows : (shift + 1) * rows].astype(jnp.bfloat16)
        total = total + chip_shift(piece, chips, chips - shift).astype(jnp.float32)
    return total


def local_order(values, n_fs, halve):
    if not halve:
        return values
    group, at = lax.axis_index("grp"), lax.axis_index("fs")
    blocks = values.reshape(values.shape[0], n_fs, 2, -1)
    mine = lax.dynamic_index_in_dim(blocks, group, 2, keepdims=False)
    other = lax.dynamic_index_in_dim(blocks, 1 - group, 2, keepdims=False)
    other = lax.dynamic_slice_in_dim(jnp.concatenate([other, other], axis=1), at, n_fs, 1)
    return jnp.concatenate([mine, other], axis=1).reshape(values.shape)


def whole_order(values, n_fs, halve):
    if not halve:
        return values
    group, at = lax.axis_index("grp"), lax.axis_index("fs")
    blocks = values.reshape(values.shape[0], 2, n_fs, -1)
    mine, other = blocks[:, 0], blocks[:, 1]
    other = lax.dynamic_slice_in_dim(
        jnp.concatenate([other, other], axis=1), (n_fs - at) % n_fs, n_fs, 1
    )
    first = jnp.where(group == 0, mine, other)
    second = jnp.where(group == 0, other, mine)
    return jnp.stack([first, second], axis=2).reshape(values.shape)


def fetch(weight, axis, halve, n_fs, name):
    if not halve:
        return [lax.all_gather(weight, "fs", axis=0, tiled=False)]
    group, at = lax.axis_index("grp"), lax.axis_index("fs")
    half = weight.shape[axis] // 2
    mine = lax.dynamic_slice_in_dim(weight, group * half, half, axis)
    other = lax.dynamic_slice_in_dim(weight, (1 - group) * half, half, axis)
    gathered = lax.all_gather(mine, "fs", axis=0, tiled=False)
    if int(name[1:]) % 2:
        rows = gathered.shape[1]
        lines = flat(gathered)
        lines = jnp.concatenate([lines, lines[: (n_fs - 2) * rows]], axis=0)
        start = (at + 1) % n_fs * rows
        sent = lax.dynamic_slice_in_dim(lines, start, (n_fs - 1) * rows, 0)
    else:
        sent = jnp.stack(
            [
                lax.dynamic_index_in_dim(gathered, (at + step) % n_fs, 0, keepdims=False)
                for step in range(1, n_fs)
            ]
        )
    received = lax.ppermute(sent, "grp", [(0, 1), (1, 0)])
    received = received.reshape(n_fs - 1, *other.shape)
    return [gathered, jnp.concatenate([other[None], received], axis=0)]


def flat(stacked):
    return stacked.reshape(-1, stacked.shape[-1])


def split_matmul(rows, parts):
    total, at = None, 0
    for part in map(flat, parts):
        piece = matmul(rows[:, at : at + part.shape[0]], part)
        total, at = piece if total is None else total + piece, at + part.shape[0]
    return total


def project_body(left, right, out):
    out[...] = jnp.dot(left[...], right[0], preferred_element_type=jnp.float32).astype(jnp.bfloat16)


def project(left, right, first_row, rows):
    blocks, depth, width = right.shape
    base = first_row // rows
    return pl.pallas_call(
        project_body,
        grid=(blocks,),
        in_specs=[
            pl.BlockSpec((rows, depth), lambda f: (base, 0)),
            pl.BlockSpec((1, depth, width), lambda f: (f, 0, 0)),
        ],
        out_specs=pl.BlockSpec((rows, width), lambda f: (0, f)),
        out_shape=jax.ShapeDtypeStruct((rows, blocks * width), jnp.bfloat16),
        cost_estimate=pl.CostEstimate(
            flops=2 * rows * blocks * width * depth,
            bytes_accessed=2 * (rows * depth + (rows + depth) * blocks * width),
            transcendentals=0,
        ),
    )(left, right)


def retain_body(chunks, rows, ids, rates, queries, keys, values, gain, out):
    head, here = pl.program_id(0), pl.program_id(1)
    forward, backward = rates[0, head], rates[1, head]
    row = lax.broadcasted_iota(jnp.int32, (rows, rows), 0)
    column = lax.broadcasted_iota(jnp.int32, (rows, rows), 1)
    apart = row - column
    query = queries[...]
    total = jnp.zeros((rows, DV), jnp.float32)
    for at in range(chunks):
        part = pl.ds(at * rows, rows)
        scores = lax.dot_general(
            query, keys[part, :], (((1,), (1,)), ((), ())), preferred_element_type=jnp.float32
        )
        steps = apart + (ids[here] - ids[at]) * rows
        distance = steps.astype(jnp.float32)
        decay = jnp.exp(jnp.where(steps >= 0, forward * distance, -backward * distance))
        decay = jnp.where(steps == 0, 2.0, decay) * DK**-0.5
        total = total + jnp.dot(
            (scores * decay).astype(jnp.bfloat16), values[part, :], preferred_element_type=jnp.float32
        )
    centered = total - jnp.mean(total, axis=-1, keepdims=True)
    variance = jnp.mean(centered * centered, axis=-1, keepdims=True)
    out[...] = (centered * lax.rsqrt(variance + EPS) * gain[0]).astype(jnp.bfloat16)


def retain(query_keys, values, gain, rates, ids):
    length, heads, chunks = values.shape[0], rates.shape[1], ids.shape[0]
    rows = length // chunks
    scalars = pl.BlockSpec(memory_space=pltpu.SMEM)
    return pl.pallas_call(
        functools.partial(retain_body, chunks, rows),
        grid=(heads, chunks),
        in_specs=[
            scalars,
            scalars,
            pl.BlockSpec((rows, DK), lambda h, r: (r, h)),
            pl.BlockSpec((length, DK), lambda h, r: (0, heads + h)),
            pl.BlockSpec((length, DV), lambda h, r: (0, h)),
            pl.BlockSpec((1, 1, DV), lambda h, r: (h, 0, 0)),
        ],
        out_specs=pl.BlockSpec((rows, DV), lambda h, r: (r, h)),
        out_shape=jax.ShapeDtypeStruct((length, heads * DV), jnp.bfloat16),
        cost_estimate=pl.CostEstimate(
            flops=2 * heads * length * length * (DK + DV),
            bytes_accessed=4 * heads * length * (DK + DV),
            transcendentals=heads * length * length,
        ),
        name="retain",
    )(ids, rates, query_keys, query_keys, values, gain.reshape(heads, 1, DV))


def project_sum(left, parts, chips):
    half = left.shape[0] // 2
    sums = []
    for part in parts:
        other_core = project(left, part, half, half)
        same_core = project(left, part, 0, half)
        sums.append(scatter_sum(same_core, other_core, chips))
    return jnp.concatenate(sums, axis=1)


def shards(
    n_grp,
    n_fs,
    n_tp,
    tokens,
    first_gain,
    mixer_gain,
    gate_weight,
    up_weight,
    down_weight,
    query_weight,
    key_weight,
    value_weight,
    head_gain,
    out_weight,
    log_decay,
):
    chips = n_tp // 2
    halve = n_grp == 2 and down_weight.shape[1] % 256 == 0
    gates = fetch(gate_weight, 0, halve, n_fs, "w0")
    ups = fetch(up_weight, 0, halve, n_fs, "w1")
    downs = fetch(down_weight, 1, halve, n_fs, "w2")
    both = jnp.concatenate([query_weight, key_weight], axis=1)
    query_keys = fetch(both, 0, halve, n_fs, "w3")
    values = fetch(value_weight, 0, halve, n_fs, "w4")
    outs = fetch(out_weight, 1, halve, n_fs, "w5")

    here = local_order(tokens, n_fs, halve)
    gains = local_order(jnp.stack([first_gain, mixer_gain]), n_fs, halve)
    rows = gather_rows(norm_rows(here, gains[0]), chips)
    hidden = jax.nn.silu(split_matmul(rows, gates)) * split_matmul(rows, ups)
    branch = project_sum(hidden.astype(jnp.bfloat16), downs, chips)
    after_first = (here.astype(jnp.float32) + 0.5 * branch).astype(jnp.bfloat16)

    rows = gather_rows(norm_rows(after_first, gains[1]), chips)
    projected = split_matmul(rows, query_keys).astype(jnp.bfloat16)
    retained = retain(
        projected,
        split_matmul(rows, values).astype(jnp.bfloat16),
        head_gain,
        log_decay,
        chunk_ids(chips),
    )
    branch = project_sum(retained, outs, chips)
    updated = (after_first.astype(jnp.float32) + branch).astype(jnp.bfloat16)
    return whole_order(updated, n_fs, halve)


def solution(mesh):
    placed = (
        P(("grp", "fs", "tp"), None),
        P(),
        P(),
        P("fs", "tp"),
        P("fs", "tp"),
        P("tp", "fs"),
        P("fs", "tp"),
        P("fs", "tp"),
        P("fs", "tp"),
        P("tp"),
        P("tp", "fs"),
        P(None, "tp"),
    )
    sizes = mesh.shape
    body = functools.partial(shards, sizes["grp"], sizes["fs"], sizes["tp"])
    return jax.shard_map(
        body, mesh=mesh, in_specs=placed, out_specs=P(("grp", "fs", "tp"), None), check_vma=False
    )
```
